32 devices in a mesh: ep: 16 (over z, y, x), tp: 2 (over core).
Axes of the slice: x: 2, y: 2, z: 4, core: 2. Of those that a mesh axis runs over, the one named last changes fastest.
Arguments:
- tokens: bfloat16 [512, 3072], P('ep'), may hold values from -6 to 6
- carried: float32 [512, 96, 128], P('ep', 'tp'), may hold values from -4 to 4
- decay_rate: float32 [96, 64], P('tp'), may hold values from 0.02 to 20
- frequency: float32 [96, 64], P('tp'), may hold values from 0 to 200
- log_step: float32 [96], P('tp'), may hold values from -4.6 to 0
- in_map: bfloat16 [96, 128, 16], P('tp'), may hold values from -1 to 1
- out_map: bfloat16 [96, 16, 128], P('tp'), may hold values from -0.5 to 0.5
- skip_gain: float32 [1536], P('tp'), may hold values from -4 to 4
- norm_gain: float32 [3072], replicated, may hold values from 0.1 to 1.9
- w_in: bfloat16 [3072, 1536], P(None, 'tp'), may hold values from -0.109375 to 0.109375
- w_out: bfloat16 [1536, 3072], P('tp'), may hold values from -0.15625 to 0.15625
- expert_gain: float32 [3072], replicated, may hold values from 0.1 to 1.9
- route_ids: int32 [512, 2], P('ep'), may hold values from 0 to 7, all different within a row; in each aligned block of 32 rows (0 to 31, 32 to 63, ...) at most 16 rows name the same one
- route_logit: float32 [512, 2], P('ep'), may hold values from -6 to 6
- w_gate: bfloat16 [3072, 43008], P(None, ('ep', 'tp')), may hold values from -0.109375 to 0.109375
- w_up: bfloat16 [3072, 43008], P(None, ('ep', 'tp')), may hold values from -0.109375 to 0.109375
- w_down: bfloat16 [43008, 3072], P(('ep', 'tp')), may hold values from -0.078125 to 0.078125
Outputs:
- new_tokens: bfloat16 [512, 3072], P('ep', 'tp')
- new_carried: float32 [512, 96, 128], P('ep', 'tp')
The draws below stay inside these ranges and needn't reach their ends.
Inputs may be any that keep to these rules, and one draw needn't show every extreme that they name: `route_ids`: each row names 2 different experts; within each aligned block of 32 rows (the rows of one index of ep) no expert is named by more than 16 rows, a bound that some block reaches.
All inputs are finite; a program needn't handle non-finite values.
Results may differ from the reference program's by a relative error of at most 0.014.
Values may be sent and summed in bfloat16 or wider, within the bound.
A program may use at most 128 MiB of HBM per device.

```python
import math
import jax
import jax.numpy as jnp
import numpy as np
from jax import lax

D = 3072
GROUPS = 96
CH = 16
STATE = 64
FF = 5376
EXPERTS = 8
TOP = 2
SEQ_DEV = 32
SEQS = 512
WIDTH = 1536
CAP = 16
N_TP = 2


def block_scale(rng, dims, split, low, largest):
    loudness, own = 1.0, jax.random.fold_in(rng, 6)
    for dim, shards_of in split:
        steps = jnp.exp(jax.random.uniform(jax.random.fold_in(own, dim), (shards_of,), jnp.float32, low / len(split), largest / len(split)))
        loudness = loudness * jnp.repeat(steps, dims[dim] // shards_of).reshape([-1 if axis == dim else 1 for axis in range(len(dims))])
    return loudness


def shared_out(key, own, number, rows, amount, top, most, slope):
    ranking = jax.random.permutation(key, amount)
    heavy_load, usual = load_shares(amount, rows * top, most, slope, True), load_shares(amount, rows * top, most, slope, False)
    places = jnp.arange(amount)

    def named(sizes, turn):
        used = int((sizes > 0).sum())
        fixed = max(1, used // 4)
        moved = fixed + (places - fixed + turn * (used - fixed)) % max(1, amount - fixed)
        return jnp.zeros((amount,), jnp.int32).at[ranking[jnp.where(places < fixed, places, moved)]].set(jnp.asarray(sizes, jnp.int32))

    sizes = jnp.where(number % 4 == 0, named(heavy_load, number // 4), named(usual, number - number // 4 - 1))
    mixed = jax.random.permutation(jax.random.fold_in(own, 3), amount)
    giver, sink = mixed[0:amount // 2 * 2:2], mixed[1:amount // 2 * 2:2]
    slack = jnp.minimum(sizes[giver] - 1, most - sizes[sink]) // 2
    slack = jnp.where((giver == ranking[0]) | (sink == ranking[0]) | (sizes[sink] == 0), 0, jnp.maximum(slack, 0))
    moved = jax.random.randint(jax.random.fold_in(own, 4), (amount // 2,), 0, 1 << 20) % (slack + 1)
    sizes = sizes.at[giver].add(-moved).at[sink].add(moved)
    members = jnp.searchsorted(jnp.cumsum(sizes), jnp.arange(rows * top), side="right").astype(jnp.int32)
    grid = members.reshape(top, rows).T
    grid = grid[jax.random.permutation(jax.random.fold_in(own, 1), rows)]
    turn = jax.random.randint(jax.random.fold_in(own, 2), (rows, 1), 0, top)
    return jnp.take_along_axis(grid, (jnp.arange(top)[None, :] + turn) % top, axis=1)


def load_shares(amount, total, limit, slope, full):
    loads = [(1 << 20) // math.isqrt(standing ** slope) + 1 for standing in range(1, amount + 1)]
    largest = limit if full else min(limit, max(-(-total // amount), total * loads[0] // sum(loads)))
    least = 1 if total - largest >= amount - 1 else 0
    holding, rest = [largest] + [least] * (amount - 1), total - largest - least * (amount - 1)
    while rest > 0:
        movable = [i for i in range(1, amount) if holding[i] < largest] or [i for i in range(1, amount) if holding[i] < limit]
        whole, budget = sum([loads[i] for i in movable]), rest
        for i in movable:
            extra = min(limit - holding[i], max(1, budget * loads[i] // whole), rest)
            holding[i] = holding[i] + extra
            rest = rest - extra
    return np.array(holding)


def gaussian(stream_key, dims, scale, bound, cuts=(), dtype=jnp.bfloat16):
    level = block_scale(stream_key, dims, cuts, -0.22, 0.18) if cuts else 1.0
    array = jax.random.normal(stream_key, dims, jnp.float32) * scale * level
    return jnp.minimum(jnp.maximum(array, -bound), bound).astype(dtype)


def setup_inputs(seed: int = 0) -> dict:
    arg_keys = jax.random.split(jax.random.key(seed), 18)
    tokens = gaussian(arg_keys[0], (SEQS, D), 1.0, 6.0, ((0, 16),))
    carried = gaussian(arg_keys[1], (SEQS, GROUPS, 2 * STATE), 0.5, 4.0, ((0, 16), (1, 2)), jnp.float32)
    decay_rate = jnp.clip(jnp.exp(math.log(20.0) - 6.9077553 * jax.random.uniform(arg_keys[2], (GROUPS, STATE), jnp.float32) ** block_scale(arg_keys[2], (GROUPS, STATE), ((0, 2),), -0.2, 0.2)), 0.02, 20.0)
    frequency = jnp.clip(200.0 * jax.random.uniform(arg_keys[3], (GROUPS, STATE), jnp.float32) ** block_scale(arg_keys[3], (GROUPS, STATE), ((0, 2),), -0.2, 0.2), 0.0, 200.0)
    log_step = jnp.clip(-4.6 + 4.6 * jax.random.uniform(arg_keys[4], (GROUPS,), jnp.float32) ** block_scale(arg_keys[4], (GROUPS,), ((0, 2),), -0.2, 0.2), -4.6, 0.0)
    in_map = gaussian(arg_keys[5], (GROUPS, 2 * STATE, CH), (2 * CH) ** -0.5, 1.0, ((0, 2),))
    out_map = gaussian(arg_keys[6], (GROUPS, CH, 2 * STATE), (2 * STATE) ** -0.5, 0.5, ((0, 2),))
    skip_gain = gaussian(arg_keys[7], (WIDTH,), 1.0, 4.0, ((0, 2),), jnp.float32)
    norm_gain = jnp.clip(1.0 + 0.18 * jax.random.normal(arg_keys[8], (D,), jnp.float32), 0.1, 1.9)
    w_in = gaussian(arg_keys[9], (D, WIDTH), D ** -0.5, 0.109375, ((1, 2),))
    w_out = gaussian(arg_keys[10], (WIDTH, D), WIDTH ** -0.5, 0.15625, ((0, 2),))
    expert_gain = jnp.clip(1.0 + 0.18 * jax.random.normal(arg_keys[11], (D,), jnp.float32), 0.1, 1.9)
    route_ids_keys = jax.random.split(jax.random.fold_in(arg_keys[12], 1), SEQS // SEQ_DEV)
    route_ids_turns = jax.random.permutation(jax.random.fold_in(arg_keys[12], 3), SEQS // SEQ_DEV)
    route_ids = jax.vmap(lambda own, number: shared_out(jax.random.fold_in(arg_keys[12], 2), own, number, SEQ_DEV, EXPERTS, TOP, CAP, 1))(route_ids_keys, route_ids_turns).reshape((SEQS, TOP))
    route_logit = gaussian(arg_keys[13], (SEQS, TOP), 1.5, 6.0, ((0, 16),), jnp.float32)
    w_gate = gaussian(arg_keys[14], (D, EXPERTS * FF), D ** -0.5, 0.109375, ((1, 32),))
    w_up = gaussian(arg_keys[15], (D, EXPERTS * FF), D ** -0.5, 0.109375, ((1, 32),))
    w_down = gaussian(arg_keys[16], (EXPERTS * FF, D), FF ** -0.5, 0.078125, ((0, 32),))
    return dict(tokens=tokens, carried=carried, decay_rate=decay_rate, frequency=frequency, log_step=log_step, in_map=in_map, out_map=out_map, skip_gain=skip_gain, norm_gain=norm_gain, w_in=w_in, w_out=w_out, expert_gain=expert_gain, route_ids=route_ids, route_logit=route_logit, w_gate=w_gate, w_up=w_up, w_down=w_down)


def normalize(rows, gain):
    wide = rows.astype(jnp.float32)
    scaled = wide * lax.rsqrt(lax.optimization_barrier(jnp.mean(wide * wide, axis=-1, keepdims=True)) + 1e-06)
    return (scaled * gain).astype(jnp.bfloat16)

def state_update(drive, carried, decay_rate, frequency, log_step, in_map, out_map, skip_gain):
    count_rows, width = drive.shape
    groups, half = decay_rate.shape
    channels = width // groups
    step_size = jnp.exp(log_step)[:, None]
    magnitude = jnp.exp(-decay_rate * step_size)
    real_decay = magnitude * jnp.cos(frequency * step_size)
    imag_decay = magnitude * jnp.sin(frequency * step_size)
    denom = decay_rate * decay_rate + frequency * frequency
    real_less = real_decay - 1.0
    real_factor = (-real_less * decay_rate + imag_decay * frequency) / denom
    imag_factor = (-imag_decay * decay_rate - real_less * frequency) / denom
    wide_drive = drive.astype(jnp.float32).reshape(count_rows, groups, channels)
    projected = jnp.einsum('sgh,gqh->sgq', wide_drive, in_map.astype(jnp.float32))
    real_in = projected[..., :half]
    imag_in = projected[..., half:]
    real_push = real_factor * real_in - imag_factor * imag_in
    imag_push = real_factor * imag_in + imag_factor * real_in
    real_old = carried[..., :half]
    imag_old = carried[..., half:]
    real_new = real_decay * real_old - imag_decay * imag_old + real_push
    imag_new = real_decay * imag_old + imag_decay * real_old + imag_push
    joined = jnp.concatenate([real_new, -imag_new], axis=-1)
    reading = jnp.einsum('sgq,ghq->sgh', joined, out_map.astype(jnp.float32), precision=lax.Precision.HIGHEST)
    total = reading.reshape(count_rows, width) + skip_gain * drive.astype(jnp.float32)
    activated = jax.nn.gelu(total).astype(jnp.bfloat16)
    return (activated, jnp.concatenate([real_new, imag_new], axis=-1))

def route_weights(route_logit):
    first = jax.nn.sigmoid(route_logit[:, 0] - route_logit[:, 1])
    second = jax.nn.sigmoid(route_logit[:, 1] - route_logit[:, 0])
    return jnp.stack([first, second], axis=1)

def expert_output(rows, gate_cols, up_cols, down_rows):
    gated = jnp.dot(rows, gate_cols, preferred_element_type=jnp.float32)
    upward = jnp.dot(rows, up_cols, preferred_element_type=jnp.float32)
    hidden = (jax.nn.silu(gated) * upward).astype(jnp.bfloat16)
    return jnp.dot(hidden, down_rows, preferred_element_type=jnp.float32)

def reference(tokens, carried, decay_rate, frequency, log_step, in_map, out_map, skip_gain, norm_gain, w_in, w_out, expert_gain, route_ids, route_logit, w_gate, w_up, w_down):
    normed = normalize(tokens, norm_gain)
    drive = jnp.dot(normed, w_in, preferred_element_type=jnp.float32).astype(jnp.bfloat16)
    activated, new_carried = state_update(drive, carried, decay_rate, frequency, log_step, in_map, out_map, skip_gain)
    block = activated.shape[1] // N_TP
    summed = jnp.zeros(tokens.shape, jnp.float32)
    for index in range(N_TP):
        partial_value = jnp.dot(activated[:, index * block:(index + 1) * block], w_out[index * block:(index + 1) * block], preferred_element_type=jnp.float32).astype(jnp.bfloat16)
        summed = summed + partial_value.astype(jnp.float32)
    mixed = (tokens.astype(jnp.float32) + summed).astype(jnp.bfloat16)
    expert_in = normalize(mixed, expert_gain)
    weights = route_weights(route_logit)
    hidden_units = w_gate.shape[1] // EXPERTS
    total = mixed.astype(jnp.float32)
    for expert in range(EXPERTS):
        chosen = lax.optimization_barrier(jnp.sum(jnp.where(route_ids == expert, weights, 0.0), axis=1))
        lower = expert * hidden_units
        upper = lower + hidden_units
        produced = expert_output(expert_in, w_gate[:, lower:upper], w_up[:, lower:upper], w_down[lower:upper])
        total = total + chosen[:, None] * produced
    return (total.astype(jnp.bfloat16), new_carried)
```

```python
import functools

import jax
import jax.numpy as jnp
from jax import lax
from jax.experimental import pallas as pl
from jax.experimental.pallas import tpu as pltpu
from jax.sharding import PartitionSpec as P

EXPERTS = 8
TOP = 2
CAP = 16


def normalize(rows, gain):
    wide = rows.astype(jnp.float32)
    scaled = wide * lax.rsqrt(jnp.mean(wide * wide, axis=-1, keepdims=True) + 1e-06)
    return (scaled * gain).astype(jnp.bfloat16)


def state_update(drive, carried, decay_rate, frequency, log_step, in_map, out_map, skip_gain):
    count_rows, width = drive.shape
    groups, half = decay_rate.shape
    channels = width // groups
    step_size = jnp.exp(log_step)[:, None]
    magnitude = jnp.exp(-decay_rate * step_size)
    real_decay = magnitude * jnp.cos(frequency * step_size)
    imag_decay = magnitude * jnp.sin(frequency * step_size)
    denom = decay_rate * decay_rate + frequency * frequency
    real_less = real_decay - 1.0
    real_factor = (-real_less * decay_rate + imag_decay * frequency) / denom
    imag_factor = (-imag_decay * decay_rate - real_less * frequency) / denom
    grouped_drive = drive.reshape(count_rows, groups, channels)
    projected = jnp.einsum(
        "sgh,gqh->sgq", grouped_drive, in_map, preferred_element_type=jnp.float32
    )
    real_in = projected[..., :half]
    imag_in = projected[..., half:]
    real_push = real_factor * real_in - imag_factor * imag_in
    imag_push = real_factor * imag_in + imag_factor * real_in
    real_old = carried[..., :half]
    imag_old = carried[..., half:]
    real_new = real_decay * real_old - imag_decay * imag_old + real_push
    imag_new = real_decay * imag_old + imag_decay * real_old + imag_push
    joined = jnp.concatenate([real_new, -imag_new], axis=-1)
    reading = jnp.einsum(
        "sgq,ghq->sgh", joined, out_map.astype(jnp.float32), precision=lax.Precision.HIGHEST
    )
    total = reading.reshape(count_rows, width) + skip_gain * drive.astype(jnp.float32)
    activated = jax.nn.gelu(total).astype(jnp.bfloat16)
    return (activated, jnp.concatenate([real_new, imag_new], axis=-1))


def route_weights(route_logit):
    first = jax.nn.sigmoid(route_logit[:, 0] - route_logit[:, 1])
    second = jax.nn.sigmoid(route_logit[:, 1] - route_logit[:, 0])
    return jnp.stack([first, second], axis=1)


MESH = pl.DeviceIdType.MESH
SEND_ORDER = (1, 2, 4, 6, 5, 7, 3)
WAIT_ORDER = (0, 1, 2, 4, 6, 5, 7, 3)
BACK_ORDER = (4, 6, 5, 7, 2, 3, 1)
PIECES = 3
BLOCK = 256


def dot_transposed(rows, weights):
    return lax.dot_general(
        rows, weights, (((1,), (1,)), ((), ())), preferred_element_type=jnp.float32
    )


def expert_kernel(
    group_size,
    tokens,
    activated,
    gain,
    pack,
    weight_high,
    weight_low,
    mix_hbm,
    gate_hbm,
    up_hbm,
    down_hbm,
    out,
    mix,
    gate,
    up,
    down,
    partial,
    partial_in,
    mixed_buf,
    normed_buf,
    packed,
    rows_buf,
    hidden,
    swap_out,
    swap_in,
    own_sum,
    peer_out,
    peer_in,
    back_out,
    returned,
    load_sem,
    partial_sem,
    direct_send,
    direct_recv,
    peer_send,
    peer_recv,
    core_send,
    core_recv,
    swap_send,
    swap_recv,
    sum_send,
    sum_recv,
    back_send,
    back_recv,
    local_sem,
):
    ep = lax.axis_index("ep")
    core = lax.axis_index("tp")
    expert = ep // group_size
    lane = ep % group_size
    other = 1 - core
    model_width = tokens.shape[1]
    half = model_width // 2
    hidden_units = gate_hbm.shape[0]
    sources = rows_buf.shape[1]
    total_rows = sources * CAP
    piece = half // PIECES

    def at_expert(step):
        place, bit = 0, 1
        while bit < EXPERTS:
            place = place + bit * lax.rem(expert // bit + step // bit, 2)
            bit *= 2
        return place

    def at_lane(step):
        return lax.rem(lane + step + group_size, group_size)

    mix_parts = 4
    mix_span = model_width // mix_parts
    mix_loads = []
    for part in range(mix_parts):
        span = pl.ds(part * mix_span, mix_span)
        mix_loads.append(
            pltpu.make_async_copy(mix_hbm.at[:, span], mix.at[:, span], load_sem.at[5 + part])
        )
        mix_loads[-1].start()
    loads = []
    for part in range(2):
        span = pl.ds(part * (hidden_units // 2), hidden_units // 2)
        loads.append(pltpu.make_async_copy(gate_hbm.at[span], gate.at[span], load_sem.at[2 * part]))
        loads.append(pltpu.make_async_copy(up_hbm.at[span], up.at[span], load_sem.at[2 * part + 1]))
    loads.append(pltpu.make_async_copy(down_hbm, down, load_sem.at[4]))

    barrier = pltpu.get_barrier_semaphore()
    pl.semaphore_signal(barrier, inc=1, device_id=(ep, other), device_id_type=MESH)
    for step in range(1, EXPERTS):
        target = at_expert(step) * group_size + lane
        pl.semaphore_signal(barrier, inc=1, device_id=(target, core), device_id_type=MESH)
    for step in range(1, group_size):
        target = expert * group_size + at_lane(step)
        pl.semaphore_signal(barrier, inc=1, device_id=(target, core), device_id_type=MESH)
    for part in range(mix_parts):
        span = pl.ds(part * mix_span, mix_span)
        mix_loads[part].wait()
        if part == mix_parts - 2:
            for load in loads:
                load.start()
        partial[:, span] = jnp.dot(
            activated[...], mix[:, span], preferred_element_type=jnp.float32
        ).astype(jnp.bfloat16)
    pl.semaphore_wait(barrier, EXPERTS + group_size - 1)

    def remote(source, target, send, recv, place):
        return pltpu.make_async_remote_copy(
            src_ref=source,
            dst_ref=target,
            send_sem=send,
            recv_sem=recv,
            device_id=place,
            device_id_type=MESH,
        )

    exchange = remote(partial, partial_in, partial_sem.at[0], partial_sem.at[1], (ep, other))
    exchange.start()
    exchange.wait()

    summed = partial[...].astype(jnp.float32) + partial_in[...].astype(jnp.float32)
    mixed = (tokens[...].astype(jnp.float32) + summed).astype(jnp.bfloat16)
    mixed_buf[...] = mixed
    normed_buf[...] = normalize(mixed, gain[...])
    own_columns = pl.ds(pl.multiple_of(core * half, 128), half)
    chosen = jnp.dot(pack[...], normed_buf[:, own_columns], preferred_element_type=jnp.float32)
    packed[...] = chosen.astype(jnp.bfloat16).reshape(EXPERTS, CAP, half)

    def direct(step):
        place = at_expert(step)
        return remote(
            packed.at[place],
            rows_buf.at[core, ep],
            direct_send.at[step],
            direct_recv.at[step],
            (place * group_size + lane, core),
        )

    def to_peer(step, shift):
        source = at_expert(step) * group_size + lane
        return remote(
            rows_buf.at[core, source],
            rows_buf.at[core, source],
            peer_send.at[shift, step],
            peer_recv.at[shift, step],
            (expert * group_size + at_lane(shift), core),
        )

    def to_core(step, shift):
        source = at_expert(step) * group_size + at_lane(-shift)
        return remote(
            rows_buf.at[core, source],
            rows_buf.at[core, source],
            core_send.at[shift, step],
            core_recv.at[shift, step],
            (ep, other),
        )

    def from_core(step, shift):
        source = at_expert(step) * group_size + at_lane(-shift)
        return remote(
            rows_buf.at[other, source],
            rows_buf.at[other, source],
            core_send.at[shift, step],
            core_recv.at[shift, step],
            (ep, other),
        )

    for step in SEND_ORDER:
        direct(step).start()
    own_copy = pltpu.make_async_copy(packed.at[expert], rows_buf.at[core, ep], local_sem)
    own_copy.start()
    for step in WAIT_ORDER:
        if step == 0:
            own_copy.wait()
        else:
            direct(step).wait_recv()
        for shift in range(1, group_size):
            to_peer(step, shift).start()
        to_core(step, 0).start()
    for step in WAIT_ORDER:
        for shift in range(1, group_size):
            to_peer(step, shift).wait_recv()
            to_core(step, shift).start()
    for step in WAIT_ORDER:
        for shift in range(group_size):
            from_core(step, shift).wait_recv()
    for load in loads[:4]:
        load.wait()

    def hidden_block(columns):
        low = rows_buf[0].reshape(total_rows, half)
        high = rows_buf[1].reshape(total_rows, half)

        def project(weights):
            return dot_transposed(low, weights[columns, :half]) + dot_transposed(
                high, weights[columns, half:]
            )

        hidden[:, columns] = (jax.nn.silu(project(gate)) * project(up)).astype(jnp.bfloat16)

    blocks = hidden_units // BLOCK

    def hidden_step(index, carry):
        hidden_block(pl.ds(pl.multiple_of(index * BLOCK, BLOCK), BLOCK))
        return carry

    lax.fori_loop(0, blocks, hidden_step, 0)
    if hidden_units % BLOCK:
        hidden_block(pl.ds(blocks * BLOCK, hidden_units % BLOCK))

    loads[4].wait()

    def produce(owner, index):
        columns = pl.ds(pl.multiple_of(owner * half + index * piece, 128), piece)
        return jnp.dot(hidden[...], down[:, columns], preferred_element_type=jnp.float32)

    def swap(index):
        return remote(
            swap_out.at[index],
            swap_in.at[index],
            swap_send.at[index],
            swap_recv.at[index],
            (ep, other),
        )

    def sum_to_peer(index, shift):
        place = at_lane(shift)
        return remote(
            peer_out.at[index, place],
            peer_in.at[index, shift - 1],
            sum_send.at[index, shift],
            sum_recv.at[index, shift],
            (expert * group_size + place, core),
        )

    def give_back(index, step):
        place = at_expert(step)
        return remote(
            back_out.at[index, place],
            returned.at[index, expert],
            back_send.at[index, step],
            back_recv.at[index, step],
            (place * group_size + lane, core),
        )

    def start_swap(index):
        swap_out[index] = produce(other, index).astype(jnp.bfloat16)
        swap(index).start()

    start_swap(0)
    for index in range(PIECES):
        if index + 1 < PIECES:
            start_swap(index + 1)
        value = produce(core, index)
        swap(index).wait_recv()
        value = value + swap_in[index].astype(jnp.float32)
        value = value.reshape(EXPERTS, group_size, CAP, piece)
        for place in range(group_size):
            own_sum[index, place] = value[:, place]
            peer_out[index, place] = value[:, place].astype(jnp.bfloat16)
        for shift in range(1, group_size):
            sum_to_peer(index, shift).start()
    for index in range(PIECES):
        value = own_sum[index, lane]
        for shift in range(1, group_size):
            sum_to_peer(index, shift).wait_recv()
            value = value + peer_in[index, shift - 1].astype(jnp.float32)
        back_out[index] = value.astype(jnp.bfloat16)
        for step in BACK_ORDER:
            give_back(index, step).start()
        returned[index, expert] = back_out[index, expert]
    for index in range(PIECES):
        for step in range(1, EXPERTS):
            give_back(index, step).wait_recv()
        rows = returned[index].reshape(EXPERTS * CAP, piece)
        value = jnp.dot(weight_high[...], rows, preferred_element_type=jnp.float32)
        value = value + jnp.dot(weight_low[...], rows, preferred_element_type=jnp.float32)
        columns = pl.ds(pl.multiple_of(core * half + index * piece, 128), piece)
        value = value + mixed_buf[:, columns].astype(jnp.float32)
        out[:, index * piece : (index + 1) * piece] = value.astype(out.dtype)

    for step in range(1, EXPERTS):
        direct(step).wait_send()
    for step in range(EXPERTS):
        for shift in range(group_size):
            to_core(step, shift).wait_send()
            if shift:
                to_peer(step, shift).wait_send()
    for index in range(PIECES):
        swap(index).wait_send()
        for shift in range(1, group_size):
            sum_to_peer(index, shift).wait_send()
        for step in range(1, EXPERTS):
            give_back(index, step).wait_send()


def experts(
    tokens, activated, gain, pack, weight_high, weight_low, w_out, w_gate, w_up, w_down
):
    count_rows, model_width = tokens.shape
    sources = lax.axis_size("ep")
    group_size = sources // EXPERTS
    half = model_width // 2
    piece = half // PIECES
    hidden_units = w_gate.shape[0]
    total_rows = sources * CAP
    peers = max(group_size - 1, 1)
    dma = pltpu.SemaphoreType.DMA
    narrow = jnp.bfloat16
    vmem = pl.BlockSpec(memory_space=pltpu.VMEM)
    anywhere = pl.BlockSpec(memory_space=pl.ANY)
    return pl.pallas_call(
        functools.partial(expert_kernel, group_size),
        out_shape=jax.ShapeDtypeStruct((count_rows, half), narrow),
        in_specs=[vmem] * 6 + [anywhere] * 4,
        out_specs=vmem,
        scratch_shapes=[
            pltpu.VMEM(w_out.shape, narrow),
            pltpu.VMEM(w_gate.shape, narrow),
            pltpu.VMEM(w_up.shape, narrow),
            pltpu.VMEM(w_down.shape, narrow),
            pltpu.VMEM((count_rows, model_width), narrow),
            pltpu.VMEM((count_rows, model_width), narrow),
            pltpu.VMEM((count_rows, model_width), narrow),
            pltpu.VMEM((count_rows, model_width), narrow),
            pltpu.VMEM((EXPERTS, CAP, half), narrow),
            pltpu.VMEM((2, sources, CAP, half), narrow),
            pltpu.VMEM((total_rows, hidden_units), narrow),
            pltpu.VMEM((PIECES, total_rows, piece), narrow),
            pltpu.VMEM((PIECES, total_rows, piece), narrow),
            pltpu.VMEM((PIECES, group_size, EXPERTS, CAP, piece), jnp.float32),
            pltpu.VMEM((PIECES, group_size, EXPERTS, CAP, piece), narrow),
            pltpu.VMEM((PIECES, peers, EXPERTS, CAP, piece), narrow),
            pltpu.VMEM((PIECES, EXPERTS, CAP, piece), narrow),
            pltpu.VMEM((PIECES, EXPERTS, CAP, piece), narrow),
            dma((9,)),
            dma((2,)),
            dma((EXPERTS,)),
            dma((EXPERTS,)),
            dma((group_size, EXPERTS)),
            dma((group_size, EXPERTS)),
            dma((group_size, EXPERTS)),
            dma((group_size, EXPERTS)),
            dma((PIECES,)),
            dma((PIECES,)),
            dma((PIECES, group_size)),
            dma((PIECES, group_size)),
            dma((PIECES, EXPERTS)),
            dma((PIECES, EXPERTS)),
            dma,
        ],
        compiler_params=pltpu.CompilerParams(
            collective_id=0, has_side_effects=True, vmem_limit_bytes=56 * 1024 * 1024
        ),
    )(tokens, activated, gain, pack, weight_high, weight_low, w_out, w_gate, w_up, w_down)


def per_device(
    tokens,
    carried,
    decay_rate,
    frequency,
    log_step,
    in_map,
    out_map,
    skip_gain,
    norm_gain,
    w_in,
    w_out,
    expert_gain,
    route_ids,
    route_logit,
    w_gate,
    w_up,
    w_down,
):
    count_rows, model_width = tokens.shape
    normed = normalize(tokens, norm_gain)
    drive = jnp.dot(normed, w_in, preferred_element_type=jnp.float32).astype(jnp.bfloat16)
    activated, new_carried = state_update(
        drive, carried, decay_rate, frequency, log_step, in_map, out_map, skip_gain
    )
    weights = route_weights(route_logit)
    expert_ids = jnp.arange(EXPERTS, dtype=jnp.int32)
    routes_flat = route_ids.reshape(-1)
    weights_flat = weights.reshape(-1)
    onehot = (routes_flat[:, None] == expert_ids[None, :]).astype(jnp.int32)
    earlier = jnp.cumsum(onehot, axis=0) - onehot
    slot_index = jnp.sum(earlier * onehot, axis=1)
    position = routes_flat * CAP + slot_index
    placement = (jnp.arange(EXPERTS * CAP, dtype=jnp.int32)[:, None] == position[None, :]).astype(
        jnp.float32
    )
    pack = placement.reshape(EXPERTS * CAP, count_rows, TOP).sum(axis=2).astype(jnp.bfloat16)
    weighing = (
        (placement * weights_flat[None, :]).reshape(EXPERTS * CAP, count_rows, TOP).sum(axis=2)
    ).T
    weight_high = lax.reduce_precision(weighing, 8, 7)
    weight_low = (weighing - weight_high).astype(jnp.bfloat16)
    weight_high = weight_high.astype(jnp.bfloat16)
    new_tokens = experts(
        tokens,
        activated,
        expert_gain.reshape(1, model_width),
        pack,
        weight_high,
        weight_low,
        w_out,
        w_gate.T,
        w_up.T,
        w_down,
    )
    return (new_tokens, new_carried)


def solution(mesh):
    return jax.shard_map(
        per_device,
        mesh=mesh,
        in_specs=(
            P("ep", None),
            P("ep", "tp", None),
            P("tp", None),
            P("tp", None),
            P("tp"),
            P("tp", None, None),
            P("tp", None, None),
            P("tp"),
            P(),
            P(None, "tp"),
            P("tp", None),
            P(),
            P("ep", None),
            P("ep", None),
            P(None, ("ep", "tp")),
            P(None, ("ep", "tp")),
            P(("ep", "tp"), None),
        ),
        out_specs=(P("ep", "tp"), P("ep", "tp", None)),
        check_vma=False,
    )
```
